32 devices in a mesh: sp: 8 (over z, x), tp: 4 (over y, core).
Axes of the slice: x: 2, y: 2, z: 4, core: 2. Of those that a mesh axis runs over, the one named last changes fastest.
Arguments:
- residual: bfloat16 [2048, 2048], P('sp', 'tp'), may hold values from -8 to 8
- query_latent: bfloat16 [2048, 512], P('sp'), may hold values from -6 to 6
- shared_latent: bfloat16 [2048, 256], P('sp'), may hold values from -6 to 6
- rotary_key: bfloat16 [2048, 32], P('sp'), may hold values from -300 to 300
- query_gain: float32 [512], replicated, may hold values from 0.1 to 1.9
- latent_gain: float32 [256], replicated, may hold values from 0.1 to 1.9
- query_narrow: bfloat16 [512, 384], P(None, 'tp'), may hold values from -0.5 to 0.5
- key_narrow: bfloat16 [256, 256], P(None, 'tp'), may hold values from -0.375 to 0.375
- value_narrow: bfloat16 [256, 256], P(None, 'tp'), may hold values from -0.375 to 0.375
- query_wide: bfloat16 [512, 640], P(None, 'tp'), may hold values from -0.5 to 0.5
- key_wide: bfloat16 [256, 512], P(None, 'tp'), may hold values from -0.375 to 0.375
- value_wide: bfloat16 [256, 512], P(None, 'tp'), may hold values from -0.375 to 0.375
- output_narrow: bfloat16 [256, 2048], P('tp'), may hold values from -1.75 to 1.75
- output_wide: bfloat16 [512, 2048], P('tp'), may hold values from -1.75 to 1.75
- first_gain: float32 [2048], P('tp'), may hold values from 0.1 to 1.9
- first_bias: float32 [2048], P('tp'), may hold values from -1.5 to 1.5
- gate_weight: bfloat16 [2048, 5632], P('sp', 'tp'), may hold values from -0.125 to 0.125
- up_weight: bfloat16 [2048, 5632], P('sp', 'tp'), may hold values from -0.125 to 0.125
- down_weight: bfloat16 [5632, 2048], P('tp', 'sp'), may hold values from -0.078125 to 0.078125
- second_gain: float32 [2048], P('tp'), may hold values from 0.1 to 1.9
- second_bias: float32 [2048], P('tp'), may hold values from -1.5 to 1.5
Outputs:
- layer_out: bfloat16 [2048, 2048], P('sp', 'tp')
The draws below stay inside these ranges and needn't reach their ends.
All inputs are finite; a program needn't handle non-finite values.
Results may differ from the reference program's by a relative error of at most 0.017.
The reference program's roundings to bfloat16 on the way count: a program that leaves them out, or rounds other values in their place, can miss the bound.
Values may be sent and summed in bfloat16 or wider, within the bound.
A program may use at most 192 MiB of HBM per device.

```python
import math
import jax
import jax.numpy as jnp
from jax import lax

D = 2048
FF = 5632
QL = 512
KVL = 256
ROPE = 32
HEADS_A = 4
HEADS_B = 4
NOPE_A = 64
V_A = 64
NOPE_B = 128
V_B = 128
GRID_W = 64
TOKENS = 2048


def draw_residual(key, part):
    col_scale = jnp.exp(jnp.linspace(math.log(0.5), math.log(1.5), D))
    base = jax.random.normal(key, (TOKENS, D), dtype=jnp.float32) * col_scale
    return jnp.clip(base, -8.0, 8.0).astype(jnp.bfloat16)


def draw_rotary_key(key, part):
    base = jax.random.normal(key, (TOKENS, ROPE), dtype=jnp.float32)
    return jnp.clip(base, -300.0, 300.0).astype(jnp.bfloat16)


def block_levels(stream_key, shape, cuts, least, high):
    level = 1.0
    for dim, blocks in cuts:
        steps = jax.random.uniform(jax.random.fold_in(jax.random.fold_in(stream_key, 6), dim), (blocks,), jnp.float32, least / len(cuts), high / len(cuts))
        level = level * jnp.repeat(jnp.exp(steps), shape[dim] // blocks).reshape((-1,) + (1,) * (len(shape) - 1 - dim))
    return level


def bell_draw(rng, dims, scale, most, shards=(), kind=jnp.bfloat16):
    result = scale * jax.random.normal(rng, dims, jnp.float32)
    if shards:
        result = result * block_levels(rng, dims, shards, -0.22, 0.18)
    return jnp.clip(result, -most, most).astype(kind)


def setup_inputs(seed: int = 0) -> dict:
    seeds = jax.random.split(jax.random.key(seed), 22)
    return {
        "residual": draw_residual(jax.random.fold_in(seeds[21], 71), 0),
        "query_latent": bell_draw(seeds[1], (TOKENS, QL), 1.0, 6.0, ((0, 8),)),
        "shared_latent": bell_draw(seeds[2], (TOKENS, KVL), 1.0, 6.0, ((0, 8),)),
        "rotary_key": draw_rotary_key(jax.random.fold_in(seeds[21], 71), 0),
        "query_gain": jnp.clip(1.0 + 0.18 * jax.random.normal(seeds[4], (QL,), jnp.float32), 0.1, 1.9),
        "latent_gain": jnp.clip(1.0 + 0.18 * jax.random.normal(seeds[5], (KVL,), jnp.float32), 0.1, 1.9),
        "query_narrow": bell_draw(seeds[6], (QL, HEADS_A * (NOPE_A + ROPE)), (QL // 4) ** -0.5, 0.5, ((1, 4),)),
        "key_narrow": bell_draw(seeds[7], (KVL, HEADS_A * NOPE_A), KVL ** -0.5, 0.375, ((1, 4),)),
        "value_narrow": bell_draw(seeds[8], (KVL, HEADS_A * V_A), KVL ** -0.5, 0.375, ((1, 4),)),
        "query_wide": bell_draw(seeds[9], (QL, HEADS_B * (NOPE_B + ROPE)), (QL // 4) ** -0.5, 0.5, ((1, 4),)),
        "key_wide": bell_draw(seeds[10], (KVL, HEADS_B * NOPE_B), KVL ** -0.5, 0.375, ((1, 4),)),
        "value_wide": bell_draw(seeds[11], (KVL, HEADS_B * V_B), KVL ** -0.5, 0.375, ((1, 4),)),
        "output_narrow": bell_draw(seeds[12], (HEADS_A * V_A, D), ((HEADS_A * V_A + HEADS_B * V_B) // 64) ** -0.5, 1.75, ((0, 4),)),
        "output_wide": bell_draw(seeds[13], (HEADS_B * V_B, D), ((HEADS_A * V_A + HEADS_B * V_B) // 64) ** -0.5, 1.75, ((0, 4),)),
        "first_gain": jnp.clip(1.0 + 0.18 * jax.random.normal(seeds[14], (D,), jnp.float32), 0.1, 1.9),
        "first_bias": bell_draw(seeds[15], (D,), 0.3, 1.5, ((0, 4),), jnp.float32),
        "gate_weight": bell_draw(seeds[16], (D, FF), D ** -0.5, 0.125, ((0, 8), (1, 4))),
        "up_weight": bell_draw(seeds[17], (D, FF), D ** -0.5, 0.125, ((0, 8), (1, 4))),
        "down_weight": bell_draw(seeds[18], (FF, D), FF ** -0.5, 0.078125, ((0, 4), (1, 8))),
        "second_gain": jnp.clip(1.0 + 0.18 * jax.random.normal(seeds[19], (D,), jnp.float32), 0.1, 1.9),
        "second_bias": bell_draw(seeds[20], (D,), 0.3, 1.5, ((0, 4),), jnp.float32),
    }


EPS_ROOT = 1e-06
EPS_LAYER = 1e-05
THETA = 10000.0
DEEP_ALPHA = 2.0 ** 0.25

def rotate(half_part, angle):
    lower, upper = jnp.split(half_part, 2, axis=-1)
    cosine = jnp.cos(angle)
    sine = jnp.sin(angle)
    return jnp.concatenate([lower * cosine - upper * sine, upper * cosine + lower * sine], axis=-1)

def turn_axial(values_in, positions):
    quarter = values_in.shape[-1] // 4
    freqs = THETA ** (-(2.0 * jnp.arange(quarter, dtype=jnp.float32)) / (2 * quarter))
    row_angle = (positions // GRID_W).astype(jnp.float32)[:, None, None] * freqs
    col_angle = (positions % GRID_W).astype(jnp.float32)[:, None, None] * freqs
    first_half, second_half = jnp.split(values_in, 2, axis=-1)
    return jnp.concatenate([rotate(first_half, row_angle), rotate(second_half, col_angle)], axis=-1)

def root_scale(latent, gain):
    floated = latent.astype(jnp.float32)
    return floated * lax.rsqrt(lax.optimization_barrier(jnp.mean(floated * floated, axis=-1, keepdims=True)) + EPS_ROOT) * gain.astype(jnp.float32)

def make_query(normed, weight, plain_dim, positions):
    product = jnp.dot(normed, weight, preferred_element_type=jnp.float32)
    head_count = weight.shape[1] // (plain_dim + ROPE)
    product = product.reshape(product.shape[0], head_count, plain_dim + ROPE)
    turned = turn_axial(product[:, :, plain_dim:], positions)
    return jnp.concatenate([product[:, :, :plain_dim], turned], axis=-1).astype(jnp.bfloat16)

def attend(queries, key_rows, value_rows, rotary_rows, plain_dim):
    count, head_count, query_dim = queries.shape
    block_size = math.gcd(count, 512)
    score_scale = query_dim ** (-0.5)
    key_float = key_rows.astype(jnp.float32)
    value_float = value_rows.astype(jnp.float32)
    rotary_float = rotary_rows.astype(jnp.float32)

    def per_block(query_block):
        query_float = query_block.astype(jnp.float32)
        scores = jnp.einsum('qhd,khd->hqk', query_float[:, :, :plain_dim], key_float)
        scores = (scores + jnp.einsum('qhd,kd->hqk', query_float[:, :, plain_dim:], rotary_float)) * score_scale
        largest = lax.optimization_barrier(jnp.max(scores, axis=-1, keepdims=True))
        raised = jnp.exp(scores - largest)
        totals = lax.optimization_barrier(jnp.sum(raised, axis=-1))
        rounded = lax.optimization_barrier(raised.astype(jnp.bfloat16)).astype(jnp.float32)
        output = jnp.einsum('hqk,khd->qhd', rounded, value_float) / totals.T[:, :, None]
        return output.astype(jnp.bfloat16)
    blocks = lax.map(per_block, queries.reshape(count // block_size, block_size, head_count, query_dim))
    return blocks.reshape(count, head_count * value_rows.shape[2])

def layer_norm(summed, gain, bias):
    center = lax.optimization_barrier(jnp.mean(summed, axis=-1, keepdims=True))
    spread = lax.optimization_barrier(jnp.mean((summed - center) * (summed - center), axis=-1, keepdims=True))
    normed = (summed - center) * lax.rsqrt(spread + EPS_LAYER) * gain.astype(jnp.float32) + bias.astype(jnp.float32)
    return normed.astype(jnp.bfloat16)

def reference(residual, query_latent, shared_latent, rotary_key, query_gain, latent_gain, query_narrow, key_narrow, value_narrow, query_wide, key_wide, value_wide, output_narrow, output_wide, first_gain, first_bias, gate_weight, up_weight, down_weight, second_gain, second_bias):
    positions = jnp.arange(residual.shape[0], dtype=jnp.int32)
    query_normed = root_scale(query_latent, query_gain).astype(jnp.bfloat16)
    latent_normed = root_scale(shared_latent, latent_gain).astype(jnp.bfloat16)
    rotary_rows = turn_axial(rotary_key.astype(jnp.float32)[:, None, :], positions)[:, 0, :].astype(jnp.bfloat16)

    def group(query_weight, key_weight, value_weight, plain_dim, value_dim):
        queries = make_query(query_normed, query_weight, plain_dim, positions)
        head_count = queries.shape[1]
        key_rows = jnp.dot(latent_normed, key_weight, preferred_element_type=jnp.float32).astype(jnp.bfloat16)
        value_rows = jnp.dot(latent_normed, value_weight, preferred_element_type=jnp.float32).astype(jnp.bfloat16)
        key_rows = key_rows.reshape(key_rows.shape[0], head_count, plain_dim)
        value_rows = value_rows.reshape(value_rows.shape[0], head_count, value_dim)
        return attend(queries, key_rows, value_rows, rotary_rows, plain_dim)
    attended_narrow = group(query_narrow, key_narrow, value_narrow, NOPE_A, V_A)
    attended_wide = group(query_wide, key_wide, value_wide, NOPE_B, V_B)
    mixed = jnp.dot(attended_narrow, output_narrow, preferred_element_type=jnp.float32)
    mixed = mixed + jnp.dot(attended_wide, output_wide, preferred_element_type=jnp.float32)
    normed_first = layer_norm(DEEP_ALPHA * residual.astype(jnp.float32) + mixed, first_gain, first_bias)
    gate = jnp.dot(normed_first, gate_weight, preferred_element_type=jnp.float32)
    lifted = jnp.dot(normed_first, up_weight, preferred_element_type=jnp.float32)
    hidden = (jax.nn.silu(gate) * lifted).astype(jnp.bfloat16)
    feed = jnp.dot(hidden, down_weight, preferred_element_type=jnp.float32)
    return layer_norm(DEEP_ALPHA * normed_first.astype(jnp.float32) + feed, second_gain, second_bias)
```

```python
import jax
import jax.numpy as jnp
from jax import lax
from jax.sharding import PartitionSpec as P

ROPE = 32
NOPE_A = 64
V_A = 64
NOPE_B = 128
V_B = 128
GRID_W = 64


EPS_ROOT = 1e-06
EPS_LAYER = 1e-05
THETA = 10000.0
DEEP_ALPHA = 2.0**0.25


def rotate(half_part, angle):
    lower, upper = jnp.split(half_part, 2, axis=-1)
    cosine = jnp.cos(angle)
    sine = jnp.sin(angle)
    return jnp.concatenate([lower * cosine - upper * sine, upper * cosine + lower * sine], axis=-1)


def turn_axial(values_in, positions):
    quarter = values_in.shape[-1] // 4
    freqs = THETA ** (-(2.0 * jnp.arange(quarter, dtype=jnp.float32)) / (2 * quarter))
    row_angle = (positions // GRID_W).astype(jnp.float32)[:, None, None] * freqs
    col_angle = (positions % GRID_W).astype(jnp.float32)[:, None, None] * freqs
    first_half, second_half = jnp.split(values_in, 2, axis=-1)
    return jnp.concatenate([rotate(first_half, row_angle), rotate(second_half, col_angle)], axis=-1)


def root_scale(latent, gain):
    floated = latent.astype(jnp.float32)
    return (
        floated * lax.rsqrt(jnp.mean(floated * floated, axis=-1, keepdims=True) + EPS_ROOT) * gain
    )


def make_query(normed, weight, plain_dim, positions):
    product = jnp.dot(normed, weight, preferred_element_type=jnp.float32)
    head_count = weight.shape[1] // (plain_dim + ROPE)
    product = product.reshape(product.shape[0], head_count, plain_dim + ROPE)
    turned = turn_axial(product[:, :, plain_dim:], positions)
    return jnp.concatenate([product[:, :, :plain_dim], turned], axis=-1).astype(jnp.bfloat16)


def fresh_state(row_count, head_count, value_dim):
    largest = jnp.full((head_count, row_count), -jnp.inf, jnp.float32)
    totals = jnp.zeros((head_count, row_count), jnp.float32)
    weighted = jnp.zeros((row_count, head_count, value_dim), jnp.float32)
    return (largest, totals, weighted)


def update(state_now, queries, key_rows, value_rows, rotary_rows, plain_dim):
    largest, totals, weighted = state_now
    score_scale = queries.shape[2] ** (-0.5)
    scores = jnp.einsum(
        "qhd,khd->hqk", queries[:, :, :plain_dim], key_rows, preferred_element_type=jnp.float32
    )
    scores = scores + jnp.einsum(
        "qhd,kd->hqk", queries[:, :, plain_dim:], rotary_rows, preferred_element_type=jnp.float32
    )
    scores = scores * score_scale
    new_largest = jnp.max(scores, axis=-1)
    factor = jnp.exp(largest - new_largest)
    raised = jnp.exp(scores - new_largest[:, :, None])
    totals = totals * factor + jnp.sum(raised, axis=-1)
    added = jnp.einsum(
        "hqk,khd->qhd", raised.astype(jnp.bfloat16), value_rows, preferred_element_type=jnp.float32
    )
    weighted = weighted * factor.T[:, :, None] + added
    return (new_largest, totals, weighted)


def finish(state_now):
    largest, totals, weighted = state_now
    output = (weighted / totals.T[:, :, None]).astype(jnp.bfloat16)
    return output.reshape(output.shape[0], output.shape[1] * output.shape[2])


def finish_norm(summed, sums, squares, gain, bias, width_total):
    center = sums / width_total
    spread = squares / width_total - center * center
    normed = (summed - center[:, None]) * lax.rsqrt(spread + EPS_LAYER)[:, None]
    return (normed * gain + bias).astype(jnp.bfloat16)


def split_groups(device_count, hidden_local, width, row_count):
    best = None
    for groups in range(1, device_count + 1):
        if device_count % groups or hidden_local % groups:
            continue
        moved = 3 * width * hidden_local // groups + 2 * row_count * groups * width
        if best is None or moved < best[0]:
            best = (moved, groups)
    return best[1]


def group_shift(values_in, shift, groups, turns):
    pairs = [
        (g * turns + t, ((g + shift) % groups) * turns + t)
        for g in range(groups)
        for t in range(turns)
    ]
    return lax.ppermute(values_in, "sp", pairs)


def turn_shift(values_in, shift, groups, turns):
    pairs = [
        (g * turns + t, g * turns + (t + shift) % turns)
        for g in range(groups)
        for t in range(turns)
    ]
    return lax.ppermute(values_in, "sp", pairs)


def swap_bit(values_in, bit, size):
    return lax.ppermute(values_in, "tp", [(i, i ^ bit) for i in range(size)])


def tp_bits(size):
    return [1 << i for i in range(size.bit_length() - 1)]


def scatter_sum(terms):
    size = lax.axis_size("tp")
    me = lax.axis_index("tp")
    width = terms.shape[1] // size
    blocks = {j: terms[:, j * width : (j + 1) * width] for j in range(size)}
    for bit in tp_bits(size):
        mine = (me & bit) != 0
        low = sorted(j for j in blocks if not j & bit)
        sent = jnp.concatenate(
            [jnp.where(mine, blocks[j], blocks[j | bit]).astype(jnp.bfloat16) for j in low], axis=1
        )
        got = swap_bit(sent, bit, size)
        blocks = {
            j: jnp.where(mine, blocks[j | bit], blocks[j])
            + got[:, i * width : (i + 1) * width].astype(jnp.float32)
            for i, j in enumerate(low)
        }
    return blocks[0]


def gather_columns(block):
    size = lax.axis_size("tp")
    me = lax.axis_index("tp")
    width = block.shape[1]
    order = [0]
    rows = block
    for bit in reversed(tp_bits(size)):
        mine = (me & bit) != 0
        got = swap_bit(rows, bit, size)
        rows = jnp.concatenate([jnp.where(mine, got, rows), jnp.where(mine, rows, got)], axis=1)
        order = order + [j | bit for j in order]
    place = [order.index(j) for j in range(size)]
    return jnp.concatenate([rows[:, p * width : (p + 1) * width] for p in place], axis=1)


def body(
    residual,
    query_latent,
    shared_latent,
    rotary_key,
    query_gain,
    latent_gain,
    query_narrow,
    key_narrow,
    value_narrow,
    query_wide,
    key_wide,
    value_wide,
    output_narrow,
    output_wide,
    first_gain,
    first_bias,
    gate_weight,
    up_weight,
    down_weight,
    second_gain,
    second_bias,
):
    row_count = residual.shape[0]
    offset = lax.axis_index("sp") * row_count
    positions = offset + jnp.arange(row_count, dtype=jnp.int32)
    query_normed = root_scale(query_latent, query_gain).astype(jnp.bfloat16)
    narrow_queries = make_query(query_normed, query_narrow, NOPE_A, positions)
    wide_queries = make_query(query_normed, query_wide, NOPE_B, positions)
    narrow_heads = narrow_queries.shape[1]
    wide_heads = wide_queries.shape[1]
    start_state = (
        fresh_state(row_count, narrow_heads, V_A),
        fresh_state(row_count, wide_heads, V_B),
    )
    device_count = lax.axis_size("sp")
    hidden_local = gate_weight.shape[1]
    width_total = residual.shape[1] * lax.axis_size("tp")
    groups = split_groups(device_count, hidden_local, width_total, row_count)
    turns = device_count // groups
    me = lax.axis_index("sp")
    my_group = me // turns
    my_turn = me % turns

    def spread(pieces):
        found = []
        for k, piece in enumerate(pieces):
            held = piece if k == 0 else group_shift(piece, k, groups, turns)
            source = (my_group - k) % groups
            found.append((source * turns + my_turn, held))
            for j in range(1, turns):
                found.append(
                    (source * turns + (my_turn - j) % turns, turn_shift(held, j, groups, turns))
                )
        return found

    latent_width = shared_latent.shape[1]
    packed = jnp.concatenate([shared_latent, rotary_key], axis=1)
    all_rows = jnp.zeros((device_count * row_count, packed.shape[1]), packed.dtype)
    for source, piece in spread([packed] * groups):
        all_rows = lax.dynamic_update_slice(all_rows, piece, (source * row_count, 0))
    all_rows, gate_weight, up_weight, down_weight = lax.optimization_barrier(
        (all_rows, gate_weight, up_weight, down_weight)
    )
    shard_rows = (all_rows[:, :latent_width], all_rows[:, latent_width:])

    hidden_count = hidden_local // groups
    depth = gate_weight.shape[0]
    down_width = down_weight.shape[1]
    first_pieces = []
    down_pieces = []
    for k in range(groups):
        start = ((my_group + k) % groups) * hidden_count
        first_pieces.append(
            jnp.stack(
                [
                    lax.dynamic_slice(gate_weight, (0, start), (depth, hidden_count)),
                    lax.dynamic_slice(up_weight, (0, start), (depth, hidden_count)),
                ]
            )
        )
        down_pieces.append(lax.dynamic_slice(down_weight, (start, 0), (hidden_count, down_width)))
    first_full = jnp.zeros((2, device_count * depth, hidden_count), gate_weight.dtype)
    for source, piece in spread(first_pieces):
        first_full = lax.dynamic_update_slice(first_full, piece, (0, source * depth, 0))
    down_full = jnp.zeros((hidden_count, device_count * down_width), down_weight.dtype)
    for source, piece in spread(down_pieces):
        down_full = lax.dynamic_update_slice(down_full, piece, (0, source * down_width))

    latent_rows = shard_rows[0]
    normed = root_scale(latent_rows, latent_gain).astype(jnp.bfloat16)
    count = latent_rows.shape[0]
    narrow_keys = jnp.dot(normed, key_narrow, preferred_element_type=jnp.float32).astype(
        jnp.bfloat16
    )
    narrow_vals = jnp.dot(normed, value_narrow, preferred_element_type=jnp.float32).astype(
        jnp.bfloat16
    )
    wide_keys = jnp.dot(normed, key_wide, preferred_element_type=jnp.float32).astype(jnp.bfloat16)
    wide_vals = jnp.dot(normed, value_wide, preferred_element_type=jnp.float32).astype(jnp.bfloat16)
    key_positions = jnp.arange(count, dtype=jnp.int32)
    rotated = turn_axial(shard_rows[1].astype(jnp.float32)[:, None, :], key_positions)[
        :, 0, :
    ].astype(jnp.bfloat16)
    count = rotated.shape[0]
    narrow_state = update(
        start_state[0],
        narrow_queries,
        narrow_keys.reshape(count, narrow_heads, NOPE_A),
        narrow_vals.reshape(count, narrow_heads, V_A),
        rotated,
        NOPE_A,
    )
    wide_state = update(
        start_state[1],
        wide_queries,
        wide_keys.reshape(count, wide_heads, NOPE_B),
        wide_vals.reshape(count, wide_heads, V_B),
        rotated,
        NOPE_B,
    )
    narrow_out = finish(narrow_state)
    wide_out = finish(wide_state)
    terms = jnp.dot(narrow_out, output_narrow, preferred_element_type=jnp.float32)
    terms = terms + jnp.dot(wide_out, output_wide, preferred_element_type=jnp.float32)
    mixed = scatter_sum(terms)
    summed = DEEP_ALPHA * residual.astype(jnp.float32) + mixed
    sums, squares = lax.psum((jnp.sum(summed, axis=1), jnp.sum(summed * summed, axis=1)), "tp")
    normed_first = finish_norm(summed, sums, squares, first_gain, first_bias, width_total)
    feed = 0.0
    for k in range(groups):
        rows = normed_first if k == 0 else group_shift(normed_first, k, groups, turns)
        full_rows = gather_columns(rows)
        gate_part = jnp.dot(full_rows, first_full[0], preferred_element_type=jnp.float32)
        lifted_part = jnp.dot(full_rows, first_full[1], preferred_element_type=jnp.float32)
        hidden = (jax.nn.silu(gate_part) * lifted_part).astype(jnp.bfloat16)
        share = scatter_sum(jnp.dot(hidden, down_full, preferred_element_type=jnp.float32))
        if k:
            share = group_shift(share.astype(jnp.bfloat16), groups - k, groups, turns)
        feed = feed + share.astype(jnp.float32)
    summed_two = DEEP_ALPHA * normed_first.astype(jnp.float32) + feed
    sums_two, squares_two = lax.psum(
        (jnp.sum(summed_two, axis=1), jnp.sum(summed_two * summed_two, axis=1)), "tp"
    )
    return finish_norm(summed_two, sums_two, squares_two, second_gain, second_bias, width_total)


def solution(mesh):
    return jax.shard_map(
        body,
        mesh=mesh,
        in_specs=(
            P("sp", "tp"),
            P("sp", None),
            P("sp", None),
            P("sp", None),
            P(),
            P(),
            P(None, "tp"),
            P(None, "tp"),
            P(None, "tp"),
            P(None, "tp"),
            P(None, "tp"),
            P(None, "tp"),
            P("tp", None),
            P("tp", None),
            P("tp"),
            P("tp"),
            P("sp", "tp"),
            P("sp", "tp"),
            P("tp", "sp"),
            P("tp"),
            P("tp"),
        ),
        out_specs=P("sp", "tp"),
        check_vma=False,
    )
```

```python
import functools

import jax
import jax.numpy as jnp
from jax import lax
from jax.experimental import pallas as pl
from jax.experimental.pallas import tpu as pltpu
from jax.sharding import PartitionSpec as P

ROPE = 32
NOPE_A = 64
V_A = 64
NOPE_B = 128
V_B = 128
GRID_W = 64


EPS_ROOT = 1e-06
EPS_LAYER = 1e-05
THETA = 10000.0
DEEP_ALPHA = 2.0**0.25


def rotate(half_part, angle):
    lower, upper = jnp.split(half_part, 2, axis=-1)
    cosine = jnp.cos(angle)
    sine = jnp.sin(angle)
    return jnp.concatenate([lower * cosine - upper * sine, upper * cosine + lower * sine], axis=-1)


def turn_axial(values_in, positions):
    quarter = values_in.shape[-1] // 4
    freqs = THETA ** (-(2.0 * jnp.arange(quarter, dtype=jnp.float32)) / (2 * quarter))
    row_angle = (positions // GRID_W).astype(jnp.float32)[:, None, None] * freqs
    col_angle = (positions % GRID_W).astype(jnp.float32)[:, None, None] * freqs
    first_half, second_half = jnp.split(values_in, 2, axis=-1)
    return jnp.concatenate([rotate(first_half, row_angle), rotate(second_half, col_angle)], axis=-1)


def root_scale(latent, gain):
    floated = latent.astype(jnp.float32)
    return (
        floated * lax.rsqrt(jnp.mean(floated * floated, axis=-1, keepdims=True) + EPS_ROOT) * gain
    )


def make_query(normed, weight, plain_dim, positions):
    product = jnp.dot(normed, weight, preferred_element_type=jnp.float32)
    head_count = weight.shape[1] // (plain_dim + ROPE)
    product = product.reshape(product.shape[0], head_count, plain_dim + ROPE)
    turned = turn_axial(product[:, :, plain_dim:], positions)
    return jnp.concatenate([product[:, :, :plain_dim], turned], axis=-1).astype(jnp.bfloat16)


def fresh_state(row_count, head_count, value_dim):
    largest = jnp.full((head_count, row_count), -jnp.inf, jnp.float32)
    totals = jnp.zeros((head_count, row_count), jnp.float32)
    weighted = jnp.zeros((row_count, head_count, value_dim), jnp.float32)
    return (largest, totals, weighted)


def update(state_now, queries, key_rows, value_rows, rotary_rows, plain_dim):
    largest, totals, weighted = state_now
    score_scale = queries.shape[2] ** (-0.5)
    scores = jnp.einsum(
        "qhd,khd->hqk", queries[:, :, :plain_dim], key_rows, preferred_element_type=jnp.float32
    )
    scores = scores + jnp.einsum(
        "qhd,kd->hqk", queries[:, :, plain_dim:], rotary_rows, preferred_element_type=jnp.float32
    )
    scores = scores * score_scale
    new_largest = jnp.max(scores, axis=-1)
    factor = jnp.exp(largest - new_largest)
    raised = jnp.exp(scores - new_largest[:, :, None])
    totals = totals * factor + jnp.sum(raised, axis=-1)
    added = jnp.einsum(
        "hqk,khd->qhd", raised.astype(jnp.bfloat16), value_rows, preferred_element_type=jnp.float32
    )
    weighted = weighted * factor.T[:, :, None] + added
    return (new_largest, totals, weighted)


def finish(state_now):
    largest, totals, weighted = state_now
    output = (weighted / totals.T[:, :, None]).astype(jnp.bfloat16)
    return output.reshape(output.shape[0], output.shape[1] * output.shape[2])


def finish_norm(summed, sums, squares, gain, bias, width_total):
    center = sums / width_total
    spread = squares / width_total - center * center
    normed = (summed - center[:, None]) * lax.rsqrt(spread + EPS_LAYER)[:, None]
    return (normed * gain + bias).astype(jnp.bfloat16)


def split_groups(device_count, hidden_local, width, row_count):
    best = None
    for groups in range(1, device_count + 1):
        if device_count % groups or hidden_local % groups:
            continue
        moved = 3 * width * hidden_local // groups + 2 * row_count * groups * width
        if best is None or moved < best[0]:
            best = (moved, groups)
    return best[1]


def group_shift(values_in, shift, groups, turns):
    pairs = [
        (g * turns + t, ((g + shift) % groups) * turns + t)
        for g in range(groups)
        for t in range(turns)
    ]
    return lax.ppermute(values_in, "sp", pairs)


def turn_shift(values_in, shift, groups, turns):
    pairs = [
        (g * turns + t, g * turns + (t + shift) % turns)
        for g in range(groups)
        for t in range(turns)
    ]
    return lax.ppermute(values_in, "sp", pairs)


def swap_bit(values_in, bit, size):
    return lax.ppermute(values_in, "tp", [(i, i ^ bit) for i in range(size)])


def tp_bits(size):
    return [1 << i for i in range(size.bit_length() - 1)]


def scatter_sum(terms):
    size = lax.axis_size("tp")
    me = lax.axis_index("tp")
    width = terms.shape[1] // size
    blocks = {j: terms[:, j * width : (j + 1) * width] for j in range(size)}
    for bit in tp_bits(size):
        mine = (me & bit) != 0
        low = sorted(j for j in blocks if not j & bit)
        sent = jnp.concatenate(
            [jnp.where(mine, blocks[j], blocks[j | bit]).astype(jnp.bfloat16) for j in low], axis=1
        )
        got = swap_bit(sent, bit, size)
        blocks = {
            j: jnp.where(mine, blocks[j | bit], blocks[j])
            + got[:, i * width : (i + 1) * width].astype(jnp.float32)
            for i, j in enumerate(low)
        }
    return blocks[0]


MESH = pl.DeviceIdType.MESH


def other(index, bit):
    return index + bit * (1 - 2 * ((index // bit) % 2))


def send(source, target, send_sem, recv_sem, sp, tp):
    return pltpu.make_async_remote_copy(
        src_ref=source,
        dst_ref=target,
        send_sem=send_sem,
        recv_sem=recv_sem,
        device_id={"sp": sp, "tp": tp},
        device_id_type=MESH,
    )


def greet(peers):
    barrier = pltpu.get_barrier_semaphore()
    for sp, tp in peers:
        pl.semaphore_signal(barrier, inc=1, device_id={"sp": sp, "tp": tp}, device_id_type=MESH)
    pl.semaphore_wait(barrier, len(peers))


def latent_kernel(groups, turns, own_ref, all_ref, zs, zr, xs, xr, cs, cr, local_sem):
    sp, tp = lax.axis_index("sp"), lax.axis_index("tp")
    group, turn = sp // turns, sp % turns
    mate = other(tp, 1)
    rows = own_ref.shape[0]
    half = rows // 2
    part = pl.ds(pl.multiple_of((tp % 2) * half, half), half)
    mate_part = pl.ds(pl.multiple_of((mate % 2) * half, half), half)
    local = pltpu.make_async_copy(own_ref, all_ref.at[sp], local_sem)
    local.start()
    greet(
        [(((group + k) % groups) * turns + turn, tp) for k in range(1, groups)]
        + [(group * turns + (turn + j) % turns, tp) for j in range(1, turns)]
        + [(sp, mate)]
    )
    copies = []
    for k in range(1, groups):
        target = ((group + k) % groups) * turns + turn
        copy = send(own_ref.at[part], all_ref.at[sp, part], zs.at[k], zr.at[k], target, tp)
        copy.start()
        copies.append(copy)
    held = []
    for k in range(groups):
        source = ((group - k + groups) % groups) * turns + turn
        if k:
            copies[k - 1].wait_recv()
            share = send(all_ref.at[source, part], all_ref.at[source, part], cs.at[k, 0], cr.at[k, 0], sp, mate)
            share.start()
            held.append((share, k, 0))
        for j in range(1, turns):
            block = all_ref.at[source, part] if k else own_ref.at[part]
            copy = send(
                block,
                all_ref.at[source, part],
                xs.at[k, j],
                xr.at[k, j],
                group * turns + (turn + j) % turns,
                tp,
            )
            copy.start()
            copies.append(copy)
    for k in range(groups):
        for j in range(1, turns):
            source = ((group - k + groups) % groups) * turns + (turn - j + turns) % turns
            copies[groups - 1 + k * (turns - 1) + j - 1].wait_recv()
            share = send(all_ref.at[source, part], all_ref.at[source, part], cs.at[k, j], cr.at[k, j], sp, mate)
            share.start()
            held.append((share, k, j))
    for copy in copies:
        copy.wait_send()
    for share, _, _ in held:
        share.wait_send()
        share.wait_recv()
    local.wait()


def gather_latents(packed, groups, turns, count):
    dma = pltpu.SemaphoreType.DMA
    return pl.pallas_call(
        functools.partial(latent_kernel, groups, turns),
        out_shape=jax.ShapeDtypeStruct((count,) + packed.shape, packed.dtype),
        in_specs=[pl.BlockSpec(memory_space=pltpu.VMEM)],
        out_specs=pl.BlockSpec(memory_space=pltpu.VMEM),
        scratch_shapes=[
            dma((groups,)),
            dma((groups,)),
            dma((groups, turns)),
            dma((groups, turns)),
            dma((groups, turns)),
            dma((groups, turns)),
            dma(()),
        ],
        compiler_params=pltpu.CompilerParams(
            collective_id=0, has_side_effects=True, vmem_limit_bytes=32 * 2**20
        ),
        name="latents",
    )(packed)


def feed_kernel(groups, turns, count, parts, x_ref, *refs):
    w_refs, (out_ref, full, weights, kept, s1, r1, s2, r2, s3, r3) = refs[:count], refs[count : count + 10]
    zs, zr, gs, gr, ps, pr, qs, qr, us, ur, ws, ls = refs[count + 10 :]
    sp, tp = lax.axis_index("sp"), lax.axis_index("tp")
    group, turn = sp // turns, sp % turns
    low, high = tp % 2, tp // 2
    near, far = other(tp, 1), other(tp, 2)
    width = x_ref.shape[1]
    per = count // parts

    loads = []
    for i in range(count):
        k, j = i // turns, i % turns
        source = ((group - k + groups) % groups) * turns + (turn - j + turns) % turns
        load = pltpu.make_async_copy(w_refs[i], weights.at[:, source], ws.at[i])
        load.start()
        loads.append(load)
    local = pltpu.make_async_copy(x_ref, full.at[0, tp], ls)
    local.start()
    greet(
        [(((group + k) % groups) * turns + turn, tp) for k in range(1, groups)]
        + [(sp, near), (sp, far)]
    )
    ahead = [None]
    for k in range(1, groups):
        copy = send(
            x_ref, full.at[k, tp], zs.at[k], zr.at[k], ((group + k) % groups) * turns + turn, tp
        )
        copy.start()
        ahead.append(copy)
    across, beside, passed = [], [], []

    def relay(k):
        if k:
            ahead[k].wait_recv()
        block = full.at[k, tp] if k else x_ref
        across.append(send(block, full.at[k, tp], gs.at[k, 0], gr.at[k, 0], sp, far))
        across[k].start()
        beside.append(send(block, full.at[k, tp], gs.at[k, 1], gr.at[k, 1], sp, near))
        beside[k].start()

    def relay_far(k):
        across[k].wait_recv()
        passed.append(send(full.at[k, far], full.at[k, far], gs.at[k, 2], gr.at[k, 2], sp, near))
        passed[k].start()

    firsts, seconds, thirds = [], [], [None]

    def compute(k):
        gate = jnp.zeros((x_ref.shape[0], weights.shape[3]), jnp.float32)
        lifted = gate
        beside[k].wait_recv()
        passed[k].wait_recv()
        for j in range(parts):
            rows = full[k, j]
            span = slice(j * per, (j + 1) * per)
            gate += jnp.dot(rows, weights[0, span].reshape(width, -1), preferred_element_type=jnp.float32)
            lifted += jnp.dot(rows, weights[1, span].reshape(width, -1), preferred_element_type=jnp.float32)
        hidden = (jax.nn.silu(gate) * lifted).astype(jnp.bfloat16)

        def block(j):
            down = weights[2, pl.ds(j * per, per)].reshape(width, -1)
            return lax.dot_general(hidden, down, (((1,), (1,)), ((), ())), preferred_element_type=jnp.float32)

        for h in range(2):
            s1[k, h] = block(2 * h + 1 - low).astype(jnp.bfloat16)
        firsts.append(send(s1.at[k], r1.at[k], ps.at[k], pr.at[k], sp, near))
        firsts[k].start()
        for h in range(2):
            kept[k, h] = block(2 * h + low)

    def second(k):
        firsts[k].wait_recv()
        s2[k] = (kept[k, 1 - high] + r1[k, 1 - high].astype(jnp.float32)).astype(jnp.bfloat16)
        seconds.append(send(s2.at[k], r2.at[k], qs.at[k], qr.at[k], sp, far))
        seconds[k].start()

    def third(k):
        seconds[k].wait_recv()
        total = kept[k, high] + r1[k, high].astype(jnp.float32) + r2[k].astype(jnp.float32)
        if k == 0:
            out_ref[...] = total
        else:
            s3[k] = total.astype(jnp.bfloat16)
            owner = ((group - k + groups) % groups) * turns + turn
            thirds.append(send(s3.at[k], r3.at[k], us.at[k], ur.at[k], owner, tp))
            thirds[k].start()

    relay(0)
    relay_far(0)
    local.wait()
    for load in loads:
        load.wait()
    if groups > 1:
        relay(1)
    for k in range(groups):
        if k + 1 < groups:
            relay_far(k + 1)
        if k + 2 < groups:
            relay(k + 2)
        compute(k)
        if k >= 1:
            second(k - 1)
        if k >= 2:
            third(k - 2)
    second(groups - 1)
    if groups > 1:
        third(groups - 2)
    third(groups - 1)
    for k in range(1, groups):
        thirds[k].wait_recv()
        out_ref[...] += r3[k].astype(jnp.float32)
    for k in range(groups):
        for copy in (across[k], beside[k], passed[k], firsts[k], seconds[k]):
            copy.wait_send()
        if k:
            ahead[k].wait_send()
            thirds[k].wait_send()


def feed_sum(rows, pieces, groups, turns, parts):
    count = groups * turns
    row_count, width = rows.shape
    dma = pltpu.SemaphoreType.DMA
    hidden = pieces[0].shape[2]
    bf, shape = jnp.bfloat16, (row_count, width)
    return pl.pallas_call(
        functools.partial(feed_kernel, groups, turns, count, parts),
        out_shape=jax.ShapeDtypeStruct(shape, jnp.float32),
        in_specs=[pl.BlockSpec(memory_space=pltpu.VMEM)]
        + [pl.BlockSpec(memory_space=pl.ANY)] * count,
        out_specs=pl.BlockSpec(memory_space=pltpu.VMEM),
        scratch_shapes=[
            pltpu.VMEM((groups, parts) + shape, bf),
            pltpu.VMEM((3, count, pieces[0].shape[1], hidden), bf),
            pltpu.VMEM((groups, 2) + shape, jnp.float32),
            pltpu.VMEM((groups, 2) + shape, bf),
            pltpu.VMEM((groups, 2) + shape, bf),
            pltpu.VMEM((groups,) + shape, bf),
            pltpu.VMEM((groups,) + shape, bf),
            pltpu.VMEM((groups,) + shape, bf),
            pltpu.VMEM((groups,) + shape, bf),
            dma((groups,)),
            dma((groups,)),
            dma((groups, 3)),
            dma((groups, 3)),
            dma((groups,)),
            dma((groups,)),
            dma((groups,)),
            dma((groups,)),
            dma((groups,)),
            dma((groups,)),
            dma((count,)),
            dma(()),
        ],
        compiler_params=pltpu.CompilerParams(
            collective_id=1, has_side_effects=True, vmem_limit_bytes=56 * 2**20
        ),
        name="feed",
    )(rows, *pieces)


def body(
    residual,
    query_latent,
    shared_latent,
    rotary_key,
    query_gain,
    latent_gain,
    query_narrow,
    key_narrow,
    value_narrow,
    query_wide,
    key_wide,
    value_wide,
    output_narrow,
    output_wide,
    first_gain,
    first_bias,
    gate_weight,
    up_weight,
    down_weight,
    second_gain,
    second_bias,
):
    row_count = residual.shape[0]
    offset = lax.axis_index("sp") * row_count
    positions = offset + jnp.arange(row_count, dtype=jnp.int32)
    query_normed = root_scale(query_latent, query_gain).astype(jnp.bfloat16)
    narrow_queries = make_query(query_normed, query_narrow, NOPE_A, positions)
    wide_queries = make_query(query_normed, query_wide, NOPE_B, positions)
    narrow_heads = narrow_queries.shape[1]
    wide_heads = wide_queries.shape[1]
    start_state = (
        fresh_state(row_count, narrow_heads, V_A),
        fresh_state(row_count, wide_heads, V_B),
    )
    device_count = lax.axis_size("sp")
    hidden_local = gate_weight.shape[1]
    width_total = residual.shape[1] * lax.axis_size("tp")
    groups = split_groups(device_count, hidden_local, width_total, row_count)
    turns = device_count // groups
    me = lax.axis_index("sp")
    my_group = me // turns
    my_turn = me % turns

    def spread(pieces):
        found = []
        for k, piece in enumerate(pieces):
            held = piece if k == 0 else group_shift(piece, k, groups, turns)
            source = (my_group - k) % groups
            found.append((source * turns + my_turn, held))
            for j in range(1, turns):
                found.append(
                    (source * turns + (my_turn - j) % turns, turn_shift(held, j, groups, turns))
                )
        return found

    latent_width = shared_latent.shape[1]
    packed = jnp.concatenate([shared_latent, rotary_key], axis=1)
    all_rows = gather_latents(packed, groups, turns, device_count)
    all_rows = all_rows.reshape(device_count * row_count, packed.shape[1])
    all_rows, gate_weight, up_weight, down_weight = lax.optimization_barrier(
        (all_rows, gate_weight, up_weight, down_weight)
    )
    shard_rows = (all_rows[:, :latent_width], all_rows[:, latent_width:])

    hidden_count = hidden_local // groups
    depth = gate_weight.shape[0]
    stacked = jnp.stack([gate_weight, up_weight, down_weight.T])
    pieces = [
        lax.dynamic_slice(
            stacked, (0, 0, ((my_group + k) % groups) * hidden_count), (3, depth, hidden_count)
        )
        for k in range(groups)
    ]
    weight_pieces = [piece for _, piece in spread(pieces)]

    latent_rows = shard_rows[0]
    normed = root_scale(latent_rows, latent_gain).astype(jnp.bfloat16)
    count = latent_rows.shape[0]
    narrow_keys = jnp.dot(normed, key_narrow, preferred_element_type=jnp.float32).astype(
        jnp.bfloat16
    )
    narrow_vals = jnp.dot(normed, value_narrow, preferred_element_type=jnp.float32).astype(
        jnp.bfloat16
    )
    wide_keys = jnp.dot(normed, key_wide, preferred_element_type=jnp.float32).astype(jnp.bfloat16)
    wide_vals = jnp.dot(normed, value_wide, preferred_element_type=jnp.float32).astype(jnp.bfloat16)
    key_positions = jnp.arange(count, dtype=jnp.int32)
    rotated = turn_axial(shard_rows[1].astype(jnp.float32)[:, None, :], key_positions)[
        :, 0, :
    ].astype(jnp.bfloat16)
    count = rotated.shape[0]
    narrow_state = update(
        start_state[0],
        narrow_queries,
        narrow_keys.reshape(count, narrow_heads, NOPE_A),
        narrow_vals.reshape(count, narrow_heads, V_A),
        rotated,
        NOPE_A,
    )
    wide_state = update(
        start_state[1],
        wide_queries,
        wide_keys.reshape(count, wide_heads, NOPE_B),
        wide_vals.reshape(count, wide_heads, V_B),
        rotated,
        NOPE_B,
    )
    narrow_out = finish(narrow_state)
    wide_out = finish(wide_state)
    terms = jnp.dot(narrow_out, output_narrow, preferred_element_type=jnp.float32)
    terms = terms + jnp.dot(wide_out, output_wide, preferred_element_type=jnp.float32)
    mixed = scatter_sum(terms)
    summed = DEEP_ALPHA * residual.astype(jnp.float32) + mixed
    sums, squares = lax.psum((jnp.sum(summed, axis=1), jnp.sum(summed * summed, axis=1)), "tp")
    normed_first = finish_norm(summed, sums, squares, first_gain, first_bias, width_total)
    feed = feed_sum(normed_first, weight_pieces, groups, turns, lax.axis_size("tp"))
    summed_two = DEEP_ALPHA * normed_first.astype(jnp.float32) + feed
    sums_two, squares_two = lax.psum(
        (jnp.sum(summed_two, axis=1), jnp.sum(summed_two * summed_two, axis=1)), "tp"
    )
    return finish_norm(summed_two, sums_two, squares_two, second_gain, second_bias, width_total)


def solution(mesh):
    return jax.shard_map(
        body,
        mesh=mesh,
        in_specs=(
            P("sp", "tp"),
            P("sp", None),
            P("sp", None),
            P("sp", None),
            P(),
            P(),
            P(None, "tp"),
            P(None, "tp"),
            P(None, "tp"),
            P(None, "tp"),
            P(None, "tp"),
            P(None, "tp"),
            P("tp", None),
            P("tp", None),
            P("tp"),
            P("tp"),
            P("sp", "tp"),
            P("sp", "tp"),
            P("tp", "sp"),
            P("tp"),
            P("tp"),
        ),
        out_specs=P("sp", "tp"),
        check_vma=False,
    )
```

```python
import functools

import jax
import jax.numpy as jnp
from jax import lax
from jax.experimental import pallas as pl
from jax.experimental.pallas import tpu as pltpu
from jax.sharding import PartitionSpec as P

ROPE = 32
NOPE_A = 64
V_A = 64
NOPE_B = 128
V_B = 128
GRID_W = 64


EPS_ROOT = 1e-06
EPS_LAYER = 1e-05
THETA = 10000.0
DEEP_ALPHA = 2.0**0.25


def rotate(half_part, angle):
    lower, upper = jnp.split(half_part, 2, axis=-1)
    cosine = jnp.cos(angle)
    sine = jnp.sin(angle)
    return jnp.concatenate([lower * cosine - upper * sine, upper * cosine + lower * sine], axis=-1)


def turn_axial(values_in, positions):
    quarter = values_in.shape[-1] // 4
    freqs = THETA ** (-(2.0 * jnp.arange(quarter, dtype=jnp.float32)) / (2 * quarter))
    row_angle = (positions // GRID_W).astype(jnp.float32)[:, None, None] * freqs
    col_angle = (positions % GRID_W).astype(jnp.float32)[:, None, None] * freqs
    first_half, second_half = jnp.split(values_in, 2, axis=-1)
    return jnp.concatenate([rotate(first_half, row_angle), rotate(second_half, col_angle)], axis=-1)


def root_scale(latent, gain):
    floated = latent.astype(jnp.float32)
    return (
        floated * lax.rsqrt(jnp.mean(floated * floated, axis=-1, keepdims=True) + EPS_ROOT) * gain
    )


def make_query(normed, weight, plain_dim, positions):
    product = jnp.dot(normed, weight, preferred_element_type=jnp.float32)
    head_count = weight.shape[1] // (plain_dim + ROPE)
    product = product.reshape(product.shape[0], head_count, plain_dim + ROPE)
    turned = turn_axial(product[:, :, plain_dim:], positions)
    return jnp.concatenate([product[:, :, :plain_dim], turned], axis=-1).astype(jnp.bfloat16)


def fresh_state(row_count, head_count, value_dim):
    largest = jnp.full((head_count, row_count), -jnp.inf, jnp.float32)
    totals = jnp.zeros((head_count, row_count), jnp.float32)
    weighted = jnp.zeros((row_count, head_count, value_dim), jnp.float32)
    return (largest, totals, weighted)


def update(state_now, queries, key_rows, value_rows, rotary_rows, plain_dim):
    largest, totals, weighted = state_now
    score_scale = queries.shape[2] ** (-0.5)
    scores = jnp.einsum(
        "qhd,khd->hqk", queries[:, :, :plain_dim], key_rows, preferred_element_type=jnp.float32
    )
    scores = scores + jnp.einsum(
        "qhd,kd->hqk", queries[:, :, plain_dim:], rotary_rows, preferred_element_type=jnp.float32
    )
    scores = scores * score_scale
    new_largest = jnp.max(scores, axis=-1)
    factor = jnp.exp(largest - new_largest)
    raised = jnp.exp(scores - new_largest[:, :, None])
    totals = totals * factor + jnp.sum(raised, axis=-1)
    added = jnp.einsum(
        "hqk,khd->qhd", raised.astype(jnp.bfloat16), value_rows, preferred_element_type=jnp.float32
    )
    weighted = weighted * factor.T[:, :, None] + added
    return (new_largest, totals, weighted)


def finish(state_now):
    largest, totals, weighted = state_now
    output = (weighted / totals.T[:, :, None]).astype(jnp.bfloat16)
    return output.reshape(output.shape[0], output.shape[1] * output.shape[2])


def finish_norm(summed, sums, squares, gain, bias, width_total):
    center = sums / width_total
    spread = squares / width_total - center * center
    normed = (summed - center[:, None]) * lax.rsqrt(spread + EPS_LAYER)[:, None]
    return (normed * gain + bias).astype(jnp.bfloat16)


def split_groups(device_count, hidden_local, width, row_count):
    best = None
    for groups in range(1, device_count + 1):
        if device_count % groups or hidden_local % groups:
            continue
        moved = 3 * width * hidden_local // groups + 2 * row_count * groups * width
        if best is None or moved < best[0]:
            best = (moved, groups)
    return best[1]


def group_shift(values_in, shift, groups, turns):
    pairs = [
        (g * turns + t, ((g + shift) % groups) * turns + t)
        for g in range(groups)
        for t in range(turns)
    ]
    return lax.ppermute(values_in, "sp", pairs)


def turn_shift(values_in, shift, groups, turns):
    pairs = [
        (g * turns + t, g * turns + (t + shift) % turns)
        for g in range(groups)
        for t in range(turns)
    ]
    return lax.ppermute(values_in, "sp", pairs)


def swap_bit(values_in, bit, size):
    return lax.ppermute(values_in, "tp", [(i, i ^ bit) for i in range(size)])


def tp_bits(size):
    return [1 << i for i in range(size.bit_length() - 1)]


def scatter_sum(terms):
    size = lax.axis_size("tp")
    me = lax.axis_index("tp")
    width = terms.shape[1] // size
    blocks = {j: terms[:, j * width : (j + 1) * width] for j in range(size)}
    for bit in tp_bits(size):
        mine = (me & bit) != 0
        low = sorted(j for j in blocks if not j & bit)
        sent = jnp.concatenate(
            [jnp.where(mine, blocks[j], blocks[j | bit]).astype(jnp.bfloat16) for j in low], axis=1
        )
        got = swap_bit(sent, bit, size)
        blocks = {
            j: jnp.where(mine, blocks[j | bit], blocks[j])
            + got[:, i * width : (i + 1) * width].astype(jnp.float32)
            for i, j in enumerate(low)
        }
    return blocks[0]


MESH = pl.DeviceIdType.MESH


def other(index, bit):
    return index + bit * (1 - 2 * ((index // bit) % 2))


def send(source, target, send_sem, recv_sem, sp, tp):
    return pltpu.make_async_remote_copy(
        src_ref=source,
        dst_ref=target,
        send_sem=send_sem,
        recv_sem=recv_sem,
        device_id={"sp": sp, "tp": tp},
        device_id_type=MESH,
    )


def greet(peers):
    barrier = pltpu.get_barrier_semaphore()
    for sp, tp in peers:
        pl.semaphore_signal(barrier, inc=1, device_id={"sp": sp, "tp": tp}, device_id_type=MESH)
    pl.semaphore_wait(barrier, len(peers))


def latent_kernel(groups, turns, own_ref, all_ref, zs, zr, xs, xr, cs, cr, local_sem):
    sp, tp = lax.axis_index("sp"), lax.axis_index("tp")
    group, turn = sp // turns, sp % turns
    mate = other(tp, 1)
    rows = own_ref.shape[0]
    half = rows // 2
    part = pl.ds(pl.multiple_of((tp % 2) * half, half), half)
    mate_part = pl.ds(pl.multiple_of((mate % 2) * half, half), half)
    local = pltpu.make_async_copy(own_ref, all_ref.at[sp], local_sem)
    local.start()
    greet(
        [(((group + k) % groups) * turns + turn, tp) for k in range(1, groups)]
        + [(group * turns + (turn + j) % turns, tp) for j in range(1, turns)]
        + [(sp, mate)]
    )
    copies = []
    for k in range(1, groups):
        target = ((group + k) % groups) * turns + turn
        copy = send(own_ref.at[part], all_ref.at[sp, part], zs.at[k], zr.at[k], target, tp)
        copy.start()
        copies.append(copy)
    held = []
    for k in range(groups):
        source = ((group - k + groups) % groups) * turns + turn
        if k:
            copies[k - 1].wait_recv()
            share = send(all_ref.at[source, part], all_ref.at[source, part], cs.at[k, 0], cr.at[k, 0], sp, mate)
            share.start()
            held.append((share, k, 0))
        for j in range(1, turns):
            block = all_ref.at[source, part] if k else own_ref.at[part]
            copy = send(
                block,
                all_ref.at[source, part],
                xs.at[k, j],
                xr.at[k, j],
                group * turns + (turn + j) % turns,
                tp,
            )
            copy.start()
            copies.append(copy)
    for k in range(groups):
        for j in range(1, turns):
            source = ((group - k + groups) % groups) * turns + (turn - j + turns) % turns
            copies[groups - 1 + k * (turns - 1) + j - 1].wait_recv()
            share = send(all_ref.at[source, part], all_ref.at[source, part], cs.at[k, j], cr.at[k, j], sp, mate)
            share.start()
            held.append((share, k, j))
    for copy in copies:
        copy.wait_send()
    for share, _, _ in held:
        share.wait_send()
        share.wait_recv()
    local.wait()


def gather_latents(packed, groups, turns, count):
    dma = pltpu.SemaphoreType.DMA
    return pl.pallas_call(
        functools.partial(latent_kernel, groups, turns),
        out_shape=jax.ShapeDtypeStruct((count,) + packed.shape, packed.dtype),
        in_specs=[pl.BlockSpec(memory_space=pltpu.VMEM)],
        out_specs=pl.BlockSpec(memory_space=pltpu.VMEM),
        scratch_shapes=[
            dma((groups,)),
            dma((groups,)),
            dma((groups, turns)),
            dma((groups, turns)),
            dma((groups, turns)),
            dma((groups, turns)),
            dma(()),
        ],
        compiler_params=pltpu.CompilerParams(
            collective_id=0, has_side_effects=True, vmem_limit_bytes=32 * 2**20
        ),
        name="latents",
    )(packed)


def across_dot(rows, columns):
    return lax.dot_general(
        rows, columns, (((1,), (1,)), ((), ())), preferred_element_type=jnp.float32
    )


def feed_kernel(groups, turns, count, parts, x_ref, *refs):
    w_refs, (out_ref, full, weights, kept, s1, r1, s2, r2, s3, r3) = refs[:count], refs[count : count + 10]
    zs, zr, gs, gr, ps, pr, qs, qr, us, ur, ws, ls = refs[count + 10 :]
    sp, tp = lax.axis_index("sp"), lax.axis_index("tp")
    group, turn = sp // turns, sp % turns
    low, high = tp % 2, tp // 2
    near, far = other(tp, 1), other(tp, 2)
    per = count // parts
    depth = x_ref.shape[1] // per

    loads = []
    for i in range(count):
        k, j = i // turns, i % turns
        source = ((group - k + groups) % groups) * turns + (turn - j + turns) % turns
        load = pltpu.make_async_copy(w_refs[i], weights.at[:, source], ws.at[i])
        load.start()
        loads.append(load)
    local = pltpu.make_async_copy(x_ref, full.at[0, tp], ls)
    local.start()
    greet(
        [(((group + k) % groups) * turns + turn, tp) for k in range(1, groups)]
        + [(sp, near), (sp, far)]
    )
    ahead = [None]
    for k in range(1, groups):
        copy = send(
            x_ref, full.at[k, tp], zs.at[k], zr.at[k], ((group + k) % groups) * turns + turn, tp
        )
        copy.start()
        ahead.append(copy)
    across, beside, passed = [], [], []

    def relay(k):
        if k:
            ahead[k].wait_recv()
        block = full.at[k, tp] if k else x_ref
        across.append(send(block, full.at[k, tp], gs.at[k, 0], gr.at[k, 0], sp, far))
        across[k].start()
        beside.append(send(block, full.at[k, tp], gs.at[k, 1], gr.at[k, 1], sp, near))
        beside[k].start()

    def relay_far(k):
        across[k].wait_recv()
        passed.append(send(full.at[k, far], full.at[k, far], gs.at[k, 2], gr.at[k, 2], sp, near))
        passed[k].start()

    firsts, seconds, thirds = [], [], [None]

    def compute(k):
        gate = jnp.zeros((x_ref.shape[0], weights.shape[2]), jnp.float32)
        lifted = gate
        beside[k].wait_recv()
        passed[k].wait_recv()
        for j in range(parts):
            rows = full[k, j]
            for i in range(per):
                piece = rows[:, i * depth : (i + 1) * depth]
                gate += across_dot(piece, weights[0, j * per + i])
                lifted += across_dot(piece, weights[1, j * per + i])
        hidden = (jax.nn.silu(gate) * lifted).astype(jnp.bfloat16)

        def block(j):
            return [
                jnp.dot(hidden, weights[2, j * per + i], preferred_element_type=jnp.float32)
                for i in range(per)
            ]

        for h in range(2):
            for i, part in enumerate(block(2 * h + 1 - low)):
                s1[k, h, :, i * depth : (i + 1) * depth] = part.astype(jnp.bfloat16)
        firsts.append(send(s1.at[k], r1.at[k], ps.at[k], pr.at[k], sp, near))
        firsts[k].start()
        for h in range(2):
            for i, part in enumerate(block(2 * h + low)):
                kept[k, h, :, i * depth : (i + 1) * depth] = part

    def second(k):
        firsts[k].wait_recv()
        s2[k] = (kept[k, 1 - high] + r1[k, 1 - high].astype(jnp.float32)).astype(jnp.bfloat16)
        seconds.append(send(s2.at[k], r2.at[k], qs.at[k], qr.at[k], sp, far))
        seconds[k].start()

    def third(k):
        seconds[k].wait_recv()
        total = kept[k, high] + r1[k, high].astype(jnp.float32) + r2[k].astype(jnp.float32)
        if k == 0:
            out_ref[...] = total
        else:
            s3[k] = total.astype(jnp.bfloat16)
            owner = ((group - k + groups) % groups) * turns + turn
            thirds.append(send(s3.at[k], r3.at[k], us.at[k], ur.at[k], owner, tp))
            thirds[k].start()

    relay(0)
    relay_far(0)
    local.wait()
    for load in loads:
        load.wait()
    if groups > 1:
        relay(1)
    for k in range(groups):
        if k + 1 < groups:
            relay_far(k + 1)
        if k + 2 < groups:
            relay(k + 2)
        compute(k)
        if k >= 1:
            second(k - 1)
        if k >= 2:
            third(k - 2)
    second(groups - 1)
    if groups > 1:
        third(groups - 2)
    third(groups - 1)
    for k in range(1, groups):
        thirds[k].wait_recv()
        out_ref[...] += r3[k].astype(jnp.float32)
    for k in range(groups):
        for copy in (across[k], beside[k], passed[k], firsts[k], seconds[k]):
            copy.wait_send()
        if k:
            ahead[k].wait_send()
            thirds[k].wait_send()


def feed_sum(rows, pieces, groups, turns, parts):
    count = groups * turns
    row_count, width = rows.shape
    dma = pltpu.SemaphoreType.DMA
    bf, shape = jnp.bfloat16, (row_count, width)
    return pl.pallas_call(
        functools.partial(feed_kernel, groups, turns, count, parts),
        out_shape=jax.ShapeDtypeStruct(shape, jnp.float32),
        in_specs=[pl.BlockSpec(memory_space=pltpu.VMEM)]
        + [pl.BlockSpec(memory_space=pl.ANY)] * count,
        out_specs=pl.BlockSpec(memory_space=pltpu.VMEM),
        scratch_shapes=[
            pltpu.VMEM((groups, parts) + shape, bf),
            pltpu.VMEM((3, count) + pieces[0].shape[1:], bf),
            pltpu.VMEM((groups, 2) + shape, jnp.float32),
            pltpu.VMEM((groups, 2) + shape, bf),
            pltpu.VMEM((groups, 2) + shape, bf),
            pltpu.VMEM((groups,) + shape, bf),
            pltpu.VMEM((groups,) + shape, bf),
            pltpu.VMEM((groups,) + shape, bf),
            pltpu.VMEM((groups,) + shape, bf),
            dma((groups,)),
            dma((groups,)),
            dma((groups, 3)),
            dma((groups, 3)),
            dma((groups,)),
            dma((groups,)),
            dma((groups,)),
            dma((groups,)),
            dma((groups,)),
            dma((groups,)),
            dma((count,)),
            dma(()),
        ],
        compiler_params=pltpu.CompilerParams(
            collective_id=1, has_side_effects=True, vmem_limit_bytes=56 * 2**20
        ),
        name="feed",
    )(rows, *pieces)


def body(
    residual,
    query_latent,
    shared_latent,
    rotary_key,
    query_gain,
    latent_gain,
    query_narrow,
    key_narrow,
    value_narrow,
    query_wide,
    key_wide,
    value_wide,
    output_narrow,
    output_wide,
    first_gain,
    first_bias,
    gate_weight,
    up_weight,
    down_weight,
    second_gain,
    second_bias,
):
    row_count = residual.shape[0]
    offset = lax.axis_index("sp") * row_count
    positions = offset + jnp.arange(row_count, dtype=jnp.int32)
    query_normed = root_scale(query_latent, query_gain).astype(jnp.bfloat16)
    narrow_queries = make_query(query_normed, query_narrow, NOPE_A, positions)
    wide_queries = make_query(query_normed, query_wide, NOPE_B, positions)
    narrow_heads = narrow_queries.shape[1]
    wide_heads = wide_queries.shape[1]
    start_state = (
        fresh_state(row_count, narrow_heads, V_A),
        fresh_state(row_count, wide_heads, V_B),
    )
    device_count = lax.axis_size("sp")
    hidden_local = gate_weight.shape[1]
    width_total = residual.shape[1] * lax.axis_size("tp")
    groups = split_groups(device_count, hidden_local, width_total, row_count)
    turns = device_count // groups
    me = lax.axis_index("sp")
    my_group = me // turns
    my_turn = me % turns

    def spread(pieces):
        found = []
        for k, piece in enumerate(pieces):
            held = piece if k == 0 else group_shift(piece, k, groups, turns)
            source = (my_group - k) % groups
            found.append((source * turns + my_turn, held))
            for j in range(1, turns):
                found.append(
                    (source * turns + (my_turn - j) % turns, turn_shift(held, j, groups, turns))
                )
        return found

    latent_width = shared_latent.shape[1]
    packed = jnp.concatenate([shared_latent, rotary_key], axis=1)
    all_rows = gather_latents(packed, groups, turns, device_count)
    all_rows = all_rows.reshape(device_count * row_count, packed.shape[1])
    hidden_count = hidden_local // groups
    depth = gate_weight.shape[0]
    stacked = jnp.stack([gate_weight.T, up_weight.T, down_weight])
    pieces = [
        lax.dynamic_slice(
            stacked, (0, ((my_group + k) % groups) * hidden_count, 0), (3, hidden_count, depth)
        )
        for k in range(groups)
    ]
    all_rows, pieces = lax.optimization_barrier((all_rows, pieces))
    weight_pieces = [piece for _, piece in spread(pieces)]

    shard_rows = (all_rows[:, :latent_width], all_rows[:, latent_width:])
    latent_rows = shard_rows[0]
    normed = root_scale(latent_rows, latent_gain).astype(jnp.bfloat16)
    count = latent_rows.shape[0]
    narrow_keys = jnp.dot(normed, key_narrow, preferred_element_type=jnp.float32).astype(
        jnp.bfloat16
    )
    narrow_vals = jnp.dot(normed, value_narrow, preferred_element_type=jnp.float32).astype(
        jnp.bfloat16
    )
    wide_keys = jnp.dot(normed, key_wide, preferred_element_type=jnp.float32).astype(jnp.bfloat16)
    wide_vals = jnp.dot(normed, value_wide, preferred_element_type=jnp.float32).astype(jnp.bfloat16)
    key_positions = jnp.arange(count, dtype=jnp.int32)
    rotated = turn_axial(shard_rows[1].astype(jnp.float32)[:, None, :], key_positions)[
        :, 0, :
    ].astype(jnp.bfloat16)
    count = rotated.shape[0]
    narrow_state = update(
        start_state[0],
        narrow_queries,
        narrow_keys.reshape(count, narrow_heads, NOPE_A),
        narrow_vals.reshape(count, narrow_heads, V_A),
        rotated,
        NOPE_A,
    )
    wide_state = update(
        start_state[1],
        wide_queries,
        wide_keys.reshape(count, wide_heads, NOPE_B),
        wide_vals.reshape(count, wide_heads, V_B),
        rotated,
        NOPE_B,
    )
    narrow_out = finish(narrow_state)
    wide_out = finish(wide_state)
    early = sorted({0, turns * min(1, groups - 1), turns * (groups - 1)} | set(range(turns)))
    narrow_out, wide_out, arrived = lax.optimization_barrier(
        (narrow_out, wide_out, [weight_pieces[i] for i in early])
    )
    for i, piece in zip(early, arrived):
        weight_pieces[i] = piece
    terms = jnp.dot(narrow_out, output_narrow, preferred_element_type=jnp.float32)
    terms = terms + jnp.dot(wide_out, output_wide, preferred_element_type=jnp.float32)
    mixed = scatter_sum(terms)
    mixed, weight_pieces[::turns] = lax.optimization_barrier((mixed, weight_pieces[::turns]))
    summed = DEEP_ALPHA * residual.astype(jnp.float32) + mixed
    sums, squares = lax.psum((jnp.sum(summed, axis=1), jnp.sum(summed * summed, axis=1)), "tp")
    normed_first = finish_norm(summed, sums, squares, first_gain, first_bias, width_total)
    feed = feed_sum(normed_first, weight_pieces, groups, turns, lax.axis_size("tp"))
    summed_two = DEEP_ALPHA * normed_first.astype(jnp.float32) + feed
    sums_two, squares_two = lax.psum(
        (jnp.sum(summed_two, axis=1), jnp.sum(summed_two * summed_two, axis=1)), "tp"
    )
    return finish_norm(summed_two, sums_two, squares_two, second_gain, second_bias, width_total)


def solution(mesh):
    return jax.shard_map(
        body,
        mesh=mesh,
        in_specs=(
            P("sp", "tp"),
            P("sp", None),
            P("sp", None),
            P("sp", None),
            P(),
            P(),
            P(None, "tp"),
            P(None, "tp"),
            P(None, "tp"),
            P(None, "tp"),
            P(None, "tp"),
            P(None, "tp"),
            P("tp", None),
            P("tp", None),
            P("tp"),
            P("tp"),
            P("sp", "tp"),
            P("sp", "tp"),
            P("tp", "sp"),
            P("tp"),
            P("tp"),
        ),
        out_specs=P("sp", "tp"),
        check_vma=False,
    )
```
